512 devices in a mesh: rep: 2 (over z_hi), fs: 32 (over z_lo, y), tp: 8 (over x, core).
Axes of the slice: x: 4, y: 4, z: 16 (z_hi: 2, z_lo: 8; z = z_hi * 8 + z_lo), core: 2. Of those that a mesh axis runs over, the one named last changes fastest.
Arguments:
- tokens_in: bfloat16 [16384, 2048], P(('rep', 'fs', 'tp')), may hold values from -6 to 6
- norm_gains: float32 [3, 2048], replicated, may hold values from 0.1 to 1.9
- gate_w: float32 [2048, 3072], P('fs', 'tp'), may hold values from -0.125 to 0.125
- gate_scale: float32 [3072], P('tp'), may hold values from 0.5 to 2
- up_w: float32 [2048, 3072], P('fs', 'tp'), may hold values from -0.125 to 0.125
- up_scale: float32 [3072], P('tp'), may hold values from 0.5 to 2
- down_w: float32 [3072, 2048], P('tp', 'fs'), may hold values from -0.109375 to 0.109375
- down_scale: float32 [2048], P('fs'), may hold values from 0.5 to 2
- query_w: float32 [2048, 2048], P('fs', 'tp'), may hold values from -0.125 to 0.125
- query_scale: float32 [2048], P('tp'), may hold values from 0.5 to 2
- key_w: float32 [2048, 2048], P('fs', 'tp'), may hold values from -0.125 to 0.125
- key_scale: float32 [2048], P('tp'), may hold values from 0.5 to 2
- value_w: float32 [2048, 2048], P('fs', 'tp'), may hold values from -0.125 to 0.125
- value_scale: float32 [2048], P('tp'), may hold values from 0.5 to 2
- out_w: float32 [2048, 2048], P('tp', 'fs'), may hold values from -0.125 to 0.125
- out_scale: float32 [2048], P('fs'), may hold values from 0.5 to 2
- head_gain: float32 [256], replicated, may hold values from 0.1 to 1.9
- decay_rate: float32 [8], P('tp'), may hold values from 0 to 1, as said below
Outputs:
- tokens_out: bfloat16 [16384, 2048], P(('rep', 'fs', 'tp'))
The draws below stay inside these ranges and needn't reach their ends.
Inputs may be any that keep to these rules, and one draw needn't show every extreme that they name: `decay_rate`: each head's decay per position, positive.
All inputs are finite; a program needn't handle non-finite values.
Results may differ from the reference program's by a relative error of at most 0.02.
Values may be sent and summed in bfloat16 or wider, within the bound.
No kernel may reach another device: no remote copies, remote signals or barrier semaphores. Data moves between devices by JAX's collectives and lax.ppermute only.
A program may use at most 64 MiB of HBM per device.

```python
import math
import jax
import jax.numpy as jnp
from jax import lax

D = 2048
FF = 3072
HEADS = 8
DK = 256
DV = 256
BLOCK = 64
SEQ = 256
TOKENS = 16384
N_TP = 8


def draw_decay_rate(key, part):
    uniform_draw = jax.random.uniform(key, (HEADS,), jnp.float32)
    lowest, highest = (0.5, 16.0)
    spread = jnp.log(highest) - jnp.log(lowest)
    return jnp.exp(jnp.log(lowest) + uniform_draw * spread) / SEQ


def steps_of(rng, shape, shards, least, high):
    level, own = 1.0, jax.random.fold_in(rng, 6)
    for dim, shards_of in shards:
        heights = jnp.exp(jax.random.uniform(jax.random.fold_in(own, dim), (shards_of,), jnp.float32, least / len(shards), high / len(shards)))
        level = level * jnp.repeat(heights, shape[dim] // shards_of).reshape([-1 if axis == dim else 1 for axis in range(len(shape))])
    return level


def noise(own_key, shape, width, most, cuts=(), held_as=jnp.bfloat16):
    drawn = jax.random.normal(own_key, shape, jnp.float32) * width
    if len(cuts) > 0:
        drawn = steps_of(own_key, shape, cuts, -0.22, 0.18) * drawn
    return jnp.clip(drawn, min=-most, max=most).astype(held_as)


def setup_inputs(seed: int = 0) -> dict:
    streams_of = jax.random.split(jax.random.key(seed), 19)
    tokens_in = noise(streams_of[0], (TOKENS, D), 1.0, 6.0, ((0, 512),))
    norm_gains = jnp.clip(1.0 + 0.18 * jax.random.normal(streams_of[1], (3, D), jnp.float32), 0.1, 1.9)
    gate_w = noise(streams_of[2], (D, FF), D ** -0.5, 0.125, ((0, 32), (1, 8)), jnp.float32)
    gate_scale = jnp.clip(jnp.exp(math.log(2.0) - 1.3862944 * jax.random.uniform(streams_of[3], (FF,), jnp.float32) ** steps_of(streams_of[3], (FF,), ((0, 8),), -0.2, 0.2)), 0.5, 2.0)
    up_w = noise(streams_of[4], (D, FF), D ** -0.5, 0.125, ((0, 32), (1, 8)), jnp.float32)
    up_scale = jnp.clip(jnp.exp(math.log(2.0) - 1.3862944 * jax.random.uniform(streams_of[5], (FF,), jnp.float32) ** steps_of(streams_of[5], (FF,), ((0, 8),), -0.2, 0.2)), 0.5, 2.0)
    down_w = noise(streams_of[6], (FF, D), FF ** -0.5, 0.109375, ((0, 8), (1, 32)), jnp.float32)
    down_scale = jnp.clip(jnp.exp(math.log(2.0) - 1.3862944 * jax.random.uniform(streams_of[7], (D,), jnp.float32) ** steps_of(streams_of[7], (D,), ((0, 32),), -0.2, 0.2)), 0.5, 2.0)
    query_w = noise(streams_of[8], (D, HEADS * DK), D ** -0.5, 0.125, ((0, 32), (1, 8)), jnp.float32)
    query_scale = jnp.clip(jnp.exp(math.log(2.0) - 1.3862944 * jax.random.uniform(streams_of[9], (HEADS * DK,), jnp.float32) ** steps_of(streams_of[9], (HEADS * DK,), ((0, 8),), -0.2, 0.2)), 0.5, 2.0)
    key_w = noise(streams_of[10], (D, HEADS * DK), D ** -0.5, 0.125, ((0, 32), (1, 8)), jnp.float32)
    key_scale = jnp.clip(jnp.exp(math.log(2.0) - 1.3862944 * jax.random.uniform(streams_of[11], (HEADS * DK,), jnp.float32) ** steps_of(streams_of[11], (HEADS * DK,), ((0, 8),), -0.2, 0.2)), 0.5, 2.0)
    value_w = noise(streams_of[12], (D, HEADS * DV), D ** -0.5, 0.125, ((0, 32), (1, 8)), jnp.float32)
    value_scale = jnp.clip(jnp.exp(math.log(2.0) - 1.3862944 * jax.random.uniform(streams_of[13], (HEADS * DV,), jnp.float32) ** steps_of(streams_of[13], (HEADS * DV,), ((0, 8),), -0.2, 0.2)), 0.5, 2.0)
    out_w = noise(streams_of[14], (HEADS * DV, D), (HEADS * DV) ** -0.5, 0.125, ((0, 8), (1, 32)), jnp.float32)
    out_scale = jnp.clip(jnp.exp(math.log(2.0) - 1.3862944 * jax.random.uniform(streams_of[15], (D,), jnp.float32) ** steps_of(streams_of[15], (D,), ((0, 32),), -0.2, 0.2)), 0.5, 2.0)
    head_gain = jnp.clip(1.0 + 0.18 * jax.random.normal(streams_of[16], (DV,), jnp.float32), 0.1, 1.9)
    decay_rate = draw_decay_rate(jax.random.fold_in(streams_of[18], 71), 0)
    return dict(tokens_in=tokens_in, norm_gains=norm_gains, gate_w=gate_w, gate_scale=gate_scale, up_w=up_w, up_scale=up_scale, down_w=down_w, down_scale=down_scale, query_w=query_w, query_scale=query_scale, key_w=key_w, key_scale=key_scale, value_w=value_w, value_scale=value_scale, out_w=out_w, out_scale=out_scale, head_gain=head_gain, decay_rate=decay_rate)


EPSILON = 1e-05

def rms_scale(stream, gain):
    return stream * lax.rsqrt(lax.optimization_barrier(jnp.mean(stream * stream, axis=-1, keepdims=True)) + EPSILON) * gain

def group_sum(hidden, weight, scale):
    groups = hidden.reshape(hidden.shape[0], N_TP, -1).transpose(1, 0, 2)
    blocks_w = weight.reshape(N_TP, -1, weight.shape[1])

    def one_group(operands):
        rounded = (jnp.dot(operands[0], operands[1], preferred_element_type=jnp.float32) * scale).astype(jnp.bfloat16)
        return lax.optimization_barrier(rounded).astype(jnp.float32)
    return lax.optimization_barrier(jnp.sum(lax.map(one_group, (groups, blocks_w)), axis=0))

def feed_forward(stream, gain, weights, scales):
    gate_b, up_b, down_b = weights
    normed = rms_scale(stream, gain).astype(jnp.bfloat16)
    gate_value = jnp.dot(normed, gate_b, preferred_element_type=jnp.float32) * scales[0]
    up_value = jnp.dot(normed, up_b, preferred_element_type=jnp.float32) * scales[1]
    hidden = (jax.nn.silu(gate_value) * up_value).astype(jnp.bfloat16)
    return group_sum(hidden, down_b, scales[2])

def retention(query, key_rows, value, decay_rate, head_gain):
    seq_len = query.shape[0]
    blocks = seq_len // BLOCK
    q_heads = query.astype(jnp.float32).reshape(blocks, BLOCK, HEADS, DK).transpose(0, 2, 1, 3)
    k_heads = key_rows.astype(jnp.float32).reshape(blocks, BLOCK, HEADS, DK).transpose(0, 2, 1, 3)
    v_heads = value.astype(jnp.float32).reshape(blocks, BLOCK, HEADS, DV).transpose(0, 2, 1, 3)
    offsets = jnp.arange(BLOCK, dtype=jnp.float32)
    inner_decay = jnp.exp(-decay_rate[:, None, None] * jnp.abs(offsets[:, None] - offsets[None, :]))
    query_decay = jnp.exp(-decay_rate[:, None] * offsets[None, :])[..., None]
    key_decay = jnp.exp(-decay_rate[:, None] * (BLOCK - offsets)[None, :])[..., None]
    block_decay = jnp.exp(-decay_rate * BLOCK)[:, None, None]

    def advance(state, inputs):
        q_blk, k_blk, v_blk = inputs
        scores = (jnp.einsum('hid,hjd->hij', q_blk, k_blk) * inner_decay).astype(jnp.bfloat16)
        scores = lax.optimization_barrier(scores).astype(jnp.float32)
        within = jnp.einsum('hij,hje->hie', scores, v_blk)
        carried = jnp.einsum('hid,hde->hie', q_blk * query_decay, state, precision=lax.Precision.HIGHEST)
        state = state * block_decay + jnp.einsum('hjd,hje->hde', k_blk * key_decay, v_blk, precision=lax.Precision.HIGHEST)
        return (state, within + carried)
    initial = jnp.zeros((HEADS, DK, DV), jnp.float32)
    _, retained = lax.scan(advance, initial, (q_heads, k_heads, v_heads))
    retained = retained.transpose(0, 2, 1, 3).reshape(seq_len, HEADS, DV)
    centred = retained - lax.optimization_barrier(jnp.mean(retained, axis=-1, keepdims=True))
    normed = centred * lax.rsqrt(lax.optimization_barrier(jnp.mean(centred * centred, axis=-1, keepdims=True)) + EPSILON) * head_gain
    return normed.reshape(seq_len, HEADS * DV).astype(jnp.bfloat16)

def reference(tokens_in, norm_gains, gate_w, gate_scale, up_w, up_scale, down_w, down_scale, query_w, query_scale, key_w, key_scale, value_w, value_scale, out_w, out_scale, head_gain, decay_rate):
    ffn_weights = (gate_w.astype(jnp.bfloat16), up_w.astype(jnp.bfloat16), down_w.astype(jnp.bfloat16))
    ffn_scales = (gate_scale, up_scale, down_scale)
    query_b = query_w.astype(jnp.bfloat16)
    key_b = key_w.astype(jnp.bfloat16)
    value_b = value_w.astype(jnp.bfloat16)
    out_b = out_w.astype(jnp.bfloat16)

    def one_sequence(stream_in):
        stream = stream_in.astype(jnp.float32)
        first = stream + 0.5 * feed_forward(stream, norm_gains[0], ffn_weights, ffn_scales)
        normed = rms_scale(first, norm_gains[1]).astype(jnp.bfloat16)
        query = (jnp.dot(normed, query_b, preferred_element_type=jnp.float32) * query_scale).astype(jnp.bfloat16)
        key_rows = (jnp.dot(normed, key_b, preferred_element_type=jnp.float32) * key_scale / math.sqrt(DK)).astype(jnp.bfloat16)
        value = (jnp.dot(normed, value_b, preferred_element_type=jnp.float32) * value_scale).astype(jnp.bfloat16)
        mixed = retention(query, key_rows, value, decay_rate, head_gain)
        second = first + group_sum(mixed, out_b, out_scale)
        final = second + 0.5 * feed_forward(second, norm_gains[2], ffn_weights, ffn_scales)
        return final.astype(jnp.bfloat16)
    sequences = tokens_in.reshape(-1, SEQ, D)
    return lax.map(one_sequence, sequences).reshape(-1, D)
```

```python
import math

import jax
import jax.numpy as jnp
from jax import lax
from jax.sharding import Mesh, PartitionSpec as P

DK = 256
DV = 256
BLOCK = 64
EPSILON = 1e-05


def gather_weights(packed):
    rep = lax.axis_index("rep")
    half = packed.shape[0] // 2
    mine = lax.dynamic_slice_in_dim(packed, rep * half, half, axis=0)
    full = lax.all_gather(mine, ("rep", "z", "y"), axis=0, tiled=True)
    return full.reshape(2, -1, half, packed.shape[1]).transpose(1, 0, 2, 3).reshape(-1, packed.shape[1])


def norm_rows(stream, gain):
    scale = lax.rsqrt(jnp.mean(stream * stream, axis=-1, keepdims=True) + EPSILON)
    return (stream * scale * gain).astype(jnp.bfloat16)


def swap_cores(array):
    return lax.ppermute(array, "core", [(0, 1), (1, 0)])


def gather_rows(rows):
    n = lax.axis_size("x")
    copies = jnp.broadcast_to(rows, (n, *rows.shape))
    own = lax.all_to_all(copies, "x", split_axis=0, concat_axis=0, tiled=True)
    own = own.reshape(-1, rows.shape[1])
    return jnp.concatenate([own, swap_cores(own)], axis=0)


def return_rows(part):
    n = lax.axis_size("x")
    half = part.shape[0] // 2
    sent = swap_cores(part[half:].astype(jnp.bfloat16))
    both = (part[:half] + sent.astype(jnp.float32)).astype(jnp.bfloat16)
    blocks = both.reshape(n, half // n, -1)
    arrived = lax.all_to_all(blocks, "x", split_axis=0, concat_axis=0, tiled=True)
    return arrived.astype(jnp.float32).sum(axis=0)


def dot(a, b):
    return jnp.dot(a, b, preferred_element_type=jnp.float32)


def dot_t(a, b):
    return lax.dot_general(a, b, (((1,), (1,)), ((), ())), preferred_element_type=jnp.float32)


def positions(rows):
    n = lax.axis_size("x")
    core = lax.axis_index("core")
    r = jnp.arange(n * rows, dtype=jnp.int32)
    first = (r // rows) * (2 * rows) + r % rows
    return jnp.concatenate([first + core * rows, first + (1 - core) * rows])


def retain(query, key_rows, value, decay_rate, head_gain, pos):
    apart = jnp.abs(pos[:, None] - pos[None, :]).astype(jnp.float32)
    seen = (pos[None, :] // BLOCK) <= (pos[:, None] // BLOCK)
    decay = jnp.where(seen, jnp.exp(-decay_rate[0] * apart), 0.0)
    scores = (dot_t(query, key_rows) * decay).astype(jnp.bfloat16)
    retained = dot(scores, value)
    centred = retained - jnp.mean(retained, axis=-1, keepdims=True)
    scale = lax.rsqrt(jnp.mean(centred * centred, axis=-1, keepdims=True) + EPSILON)
    return (centred * scale * head_gain).astype(jnp.bfloat16)


def on_device(
    tokens_in, norm_gains, gate_w, gate_scale, up_w, up_scale, down_w, down_scale,
    query_w, query_scale, key_w, key_scale, value_w, value_scale, out_w, out_scale,
    head_gain, decay_rate,
):
    def low(w):
        return w.astype(jnp.bfloat16)

    down_t = low(low(down_w).T.astype(jnp.float32) * down_scale[:, None])
    out_t = low(low(out_w).T.astype(jnp.float32) * out_scale[:, None])
    pieces = [low(gate_w), low(up_w), down_t, low(query_w), low(key_w), low(value_w), out_t]
    packed = jnp.concatenate(pieces, axis=1)
    full = gather_weights(packed)
    at, parts = 0, []
    for p in pieces:
        parts.append(full[:, at : at + p.shape[1]])
        at += p.shape[1]
    gate_f, up_f, down_f, query_f, key_f, value_f, out_f = parts

    def feed_forward(stream, gain):
        rows = gather_rows(norm_rows(stream, gain))
        gate = dot(rows, gate_f) * gate_scale
        up = dot(rows, up_f) * up_scale
        hidden = low(jax.nn.silu(gate) * up)
        return return_rows(dot_t(hidden, down_f))

    stream = tokens_in.astype(jnp.float32)
    stream = stream + 0.5 * feed_forward(stream, norm_gains[0])
    rows = gather_rows(norm_rows(stream, norm_gains[1]))
    query = low(dot(rows, query_f) * query_scale)
    key_rows = low(dot(rows, key_f) * key_scale / math.sqrt(DK))
    value = low(dot(rows, value_f) * value_scale)
    mixed = retain(query, key_rows, value, decay_rate, head_gain, positions(tokens_in.shape[0]))
    stream = stream + return_rows(dot_t(mixed, out_f))
    stream = stream + 0.5 * feed_forward(stream, norm_gains[2])
    return stream.astype(jnp.bfloat16)


def solution(mesh):
    devices = mesh.devices
    reps, fs, tp = devices.shape
    fine = Mesh(devices.reshape(reps, fs // 4, 4, tp // 2, 2), ("rep", "z", "y", "x", "core"))
    F, T = ("z", "y"), ("x", "core")
    rows = P(("rep", "z", "y", "x", "core"), None)
    wide, tall, cols, depth = P(F, T), P(T, F), P(T), P(F)
    placed = (
        rows, P(), wide, cols, wide, cols, tall, depth,
        wide, cols, wide, cols, wide, cols, tall, depth,
        P(), cols,
    )
    return jax.shard_map(on_device, mesh=fine, in_specs=placed, out_specs=rows, check_vma=False)
```

```python
import math

import jax
import jax.numpy as jnp
from jax import lax
from jax.experimental import pallas as pl
from jax.experimental.pallas import tpu as pltpu
from jax.sharding import Mesh, PartitionSpec as P

DK = 256
DV = 256
BLOCK = 64
EPSILON = 1e-05
NZ, NY, NX = 8, 4, 4
ROWS = 32
VMEM = pl.BlockSpec(memory_space=pltpu.VMEM)
SMEM = pl.BlockSpec(memory_space=pltpu.SMEM)
ANY = pl.BlockSpec(memory_space=pl.ANY)


def dot(a, b):
    return jnp.dot(a, b, preferred_element_type=jnp.float32)


def dot_t(a, b):
    return lax.dot_general(a, b, (((1,), (1,)), ((), ())), preferred_element_type=jnp.float32)


def low(w):
    return w.astype(jnp.bfloat16)


def pack_kernel(gate, up, down, ds, query, key, value, out, os, tokens, gain, ffn_ref, mix_ref, rows_ref):
    def column(row):
        n = row.shape[1]
        i = lax.broadcasted_iota(jnp.int32, (n, n), 0)
        j = lax.broadcasted_iota(jnp.int32, (n, n), 1)
        return jnp.sum(jnp.where(i == j, row, 0.0), axis=1, keepdims=True)

    def scaled(w, s):
        return low(low(w[...]).astype(jnp.float32) * column(s[...]))

    n = gate.shape[1]
    ffn_ref[:, :n] = low(gate[...])
    ffn_ref[:, n : 2 * n] = low(up[...])
    ffn_ref[:, 2 * n :] = scaled(down, ds)
    mix = (low(query[...]), low(key[...]), low(value[...]), scaled(out, os))
    for k in range(NY):
        for i, w in enumerate(mix):
            mix_ref[k, :, i * DK : (i + 1) * DK] = w
    stream = tokens[...].astype(jnp.float32)
    scale = lax.rsqrt(jnp.mean(stream * stream, axis=-1, keepdims=True) + EPSILON)
    normed = low(stream * scale * gain[...])
    for k in range(NX):
        rows_ref[k] = normed


def pack(gate, up, down, ds, query, key, value, out, os, tokens, gain):
    rows, n = gate.shape
    return pl.pallas_call(
        pack_kernel,
        out_shape=(
            jax.ShapeDtypeStruct((rows, 3 * n), jnp.bfloat16),
            jax.ShapeDtypeStruct((NY, rows, 4 * DK), jnp.bfloat16),
            jax.ShapeDtypeStruct((NX, *tokens.shape), jnp.bfloat16),
        ),
        in_specs=[VMEM] * 11,
        out_specs=(VMEM,) * 3,
        name="pack",
    )(gate, up, down, ds, query, key, value, out, os, tokens, gain)


def along_z(array, step):
    return lax.ppermute(array, ("rep", "z"), [(g, (g + step) % (2 * NZ)) for g in range(2 * NZ)])


def along_y(array, step):
    return lax.ppermute(array, "y", [(g, (g + step) % NY) for g in range(NY)])


def gather_ffn(mine):
    up, down = [mine], [mine]
    for k in range(4):
        with jax.named_scope(f"ffn_z{k}_up"):
            up.append(along_z(up[-1], 1))
        if k < 3:
            with jax.named_scope(f"ffn_z{k}_down"):
                down.append(along_z(down[-1], -1))
    arrays, owners = [], []

    def spread(name, blocks, dz, cut):
        own = jnp.stack(blocks)
        with jax.named_scope(f"ffn_{name}_up"):
            below = along_y(own, 1)
        with jax.named_scope(f"ffn_{name}_down"):
            above = along_y(own, -1)
        with jax.named_scope(f"ffn_{name}_far_up"):
            far = along_y(below[:cut], 1)
        with jax.named_scope(f"ffn_{name}_far_down"):
            far2 = along_y(above[cut:], -1)
        arrays.extend((own, below, above, far, far2))
        for dy, which in ((0, dz), (-1, dz), (1, dz), (-2, dz[:cut]), (-2, dz[cut:])):
            owners.append([(d, dy) for d in which])

    spread("y0", [mine, up[1], down[1], up[2], down[2]], [0, -1, 1, -2, 2], 3)
    spread("y1", [up[3], down[3], up[4]], [-3, 3, -4], 1)
    return arrays, owners


def gather_mix(copies):
    with jax.named_scope("mix_y"):
        mine = lax.all_to_all(copies, "y", split_axis=0, concat_axis=0, tiled=True)
    mine = mine.reshape(-1, copies.shape[2])
    up, down = [mine], [mine]
    for k in range(4):
        with jax.named_scope(f"mix_z{k}_up"):
            up.append(along_z(up[-1], 1))
        if k < 3:
            with jax.named_scope(f"mix_z{k}_down"):
                down.append(along_z(down[-1], -1))
    return up + down[1:], [0, -1, -2, -3, -4, 1, 2, 3]


def swap_cores(array):
    return lax.ppermute(array, "core", [(0, 1), (1, 0)])


def gather_rows(copies):
    own = lax.all_to_all(copies, "x", split_axis=0, concat_axis=0, tiled=True)
    own = own.reshape(-1, copies.shape[2])
    return own, swap_cores(own)


def return_rows(own, other):
    both = low(own + swap_cores(other).astype(jnp.float32))
    blocks = both.reshape(NX, -1, both.shape[1])
    arrived = lax.all_to_all(blocks, "x", split_axis=0, concat_axis=0, tiled=True)
    return arrived.astype(jnp.float32).sum(axis=0)


def norm_copies(stream, gain):
    scale = lax.rsqrt(jnp.mean(stream * stream, axis=-1, keepdims=True) + EPSILON)
    rows = low(stream * scale * gain)
    return jnp.broadcast_to(rows, (NX, *rows.shape))


def fetch(at, arrays, owners, held, sem, rows):
    copies = []
    for ref, blocks in zip(arrays, owners):
        for i, (dz, dy) in enumerate(blocks):
            row = pl.multiple_of(at(dz, dy) * rows, rows)
            src = ref.at[i] if len(ref.shape) == 3 else ref
            copies.append(pltpu.make_async_copy(src, held.at[pl.ds(row, rows)], sem.at[len(copies)]))
    for c in copies:
        c.start()
    return copies


def ffn_kernel(owners, place, own_rows, other_rows, gs, us, *rest):
    n = len(owners)
    arrays, (own_ref, other_ref, held, sem) = rest[:n], rest[n:]
    z, y = place[0], place[1]

    def at(dz, dy):
        return lax.rem(z + (NZ + dz), NZ) * NY + lax.rem(y + (NY + dy), NY)

    for c in fetch(at, arrays, owners, held, sem, held.shape[0] // (NZ * NY)):
        c.wait()
    units = held.shape[1] // 3
    rows = jnp.concatenate([own_rows[...], other_rows[...]], axis=0)
    gate = dot(rows, held[:, :units]) * gs[...]
    up = dot(rows, held[:, units : 2 * units]) * us[...]
    hidden = low(gate / (1.0 + jnp.exp(-gate)) * up)
    part = dot_t(hidden, held[:, 2 * units :])
    half = own_ref.shape[0]
    own_ref[...] = part[:half]
    other_ref[...] = low(part[half:])


def feed_forward(place, own, other, gate_scale, up_scale, arrays, owners):
    rows, wide = own.shape
    count = sum(len(o) for o in owners)
    own_part, other_part = pl.pallas_call(
        lambda *refs: ffn_kernel(owners, *refs),
        out_shape=(
            jax.ShapeDtypeStruct((rows, wide), jnp.float32),
            jax.ShapeDtypeStruct((rows, wide), jnp.bfloat16),
        ),
        in_specs=[SMEM] + [VMEM] * 4 + [ANY] * len(arrays),
        out_specs=(VMEM, VMEM),
        scratch_shapes=[
            pltpu.VMEM((wide, arrays[0].shape[-1]), jnp.bfloat16),
            pltpu.SemaphoreType.DMA((count,)),
        ],
        compiler_params=pltpu.CompilerParams(vmem_limit_bytes=40 * 1024 * 1024),
        name="ffn",
    )(place, own, other, gate_scale, up_scale, *arrays)
    return return_rows(own_part, other_part)


def mix_kernel(dzs, place, rate, own_rows, other_rows, qs, ks, vs, gain, *rest):
    n = len(dzs)
    arrays, (own_ref, other_ref, held, sem) = rest[:n], rest[n:]
    z, core = place[0], place[2]

    def at(dz, _):
        return lax.rem(z + (NZ + dz), NZ)

    owners = [[(dz, 0)] for dz in dzs]
    for c in fetch(at, arrays, owners, held, sem, held.shape[0] // NZ):
        c.wait()
    rows = jnp.concatenate([own_rows[...], other_rows[...]], axis=0)
    query = low(dot(rows, held[:, :DK]) * qs[...])
    key_rows = low(dot(rows, held[:, DK : 2 * DK]) * ks[...] / math.sqrt(DK))
    value = low(dot(rows, held[:, 2 * DK : 3 * DK]) * vs[...])

    total = rows.shape[0]

    def position(axis):
        r = lax.broadcasted_iota(jnp.int32, (total, total), axis)
        half = r // (total // 2)
        side = jnp.where(half == 0, core, 1 - core)
        return (r % (total // 2)) // ROWS * (2 * ROWS) + side * ROWS + r % ROWS

    pi, pj = position(0), position(1)
    apart = jnp.abs(pi - pj).astype(jnp.float32)
    decay = jnp.where(pj // BLOCK <= pi // BLOCK, jnp.exp(-rate[0] * apart), 0.0)
    scores = low(dot_t(query, key_rows) * decay)
    retained = dot(scores, value)
    centred = retained - jnp.mean(retained, axis=-1, keepdims=True)
    scale = lax.rsqrt(jnp.mean(centred * centred, axis=-1, keepdims=True) + EPSILON)
    mixed = low(centred * scale * gain[...])
    part = dot_t(mixed, held[:, 3 * DK :])
    half = own_ref.shape[0]
    own_ref[...] = part[:half]
    other_ref[...] = low(part[half:])


def mix(place, rate, own, other, scales, head_gain, arrays, dzs):
    rows, wide = own.shape
    own_part, other_part = pl.pallas_call(
        lambda *refs: mix_kernel(dzs, *refs),
        out_shape=(
            jax.ShapeDtypeStruct((rows, wide), jnp.float32),
            jax.ShapeDtypeStruct((rows, wide), jnp.bfloat16),
        ),
        in_specs=[SMEM, SMEM] + [VMEM] * 6 + [ANY] * len(arrays),
        out_specs=(VMEM, VMEM),
        scratch_shapes=[
            pltpu.VMEM((wide, 4 * DK), jnp.bfloat16),
            pltpu.SemaphoreType.DMA((len(arrays),)),
        ],
        compiler_params=pltpu.CompilerParams(vmem_limit_bytes=40 * 1024 * 1024),
        name="mix",
    )(place, rate, own, other, *scales, head_gain, *arrays)
    return return_rows(own_part, other_part)


def on_device(
    tokens_in, norm_gains, gate_w, gate_scale, up_w, up_scale, down_w, down_scale,
    query_w, query_scale, key_w, key_scale, value_w, value_scale, out_w, out_scale,
    head_gain, decay_rate,
):
    def row(v):
        return v.reshape(1, -1)

    place = jnp.stack([lax.axis_index(a).astype(jnp.int32) for a in ("z", "y", "core")])
    ffn_mine, mix_mine, copies = pack(
        gate_w, up_w, down_w.T, row(down_scale), query_w, key_w, value_w, out_w.T, row(out_scale),
        tokens_in, norm_gains[:1],
    )
    ffn_arrays, owners = gather_ffn(ffn_mine)
    with jax.named_scope("rows0"):
        own, other = gather_rows(copies)
    mix_arrays, dzs = gather_mix(mix_mine)
    gs, us = row(gate_scale), row(up_scale)
    scales = (row(query_scale), row(key_scale), row(value_scale))

    stream = tokens_in.astype(jnp.float32)
    stream = stream + 0.5 * feed_forward(place, own, other, gs, us, ffn_arrays, owners)
    own, other = gather_rows(norm_copies(stream, norm_gains[1]))
    stream = stream + mix(place, decay_rate, own, other, scales, row(head_gain), mix_arrays, dzs)
    own, other = gather_rows(norm_copies(stream, norm_gains[2]))
    stream = stream + 0.5 * feed_forward(place, own, other, gs, us, ffn_arrays, owners)
    return stream.astype(jnp.bfloat16)


def solution(mesh):
    devices = mesh.devices
    fine = Mesh(devices.reshape(2, NZ, NY, NX, 2), ("rep", "z", "y", "x", "core"))
    F, T = ("z", "y"), ("x", "core")
    rows = P(("rep", "z", "y", "x", "core"), None)
    wide, tall, cols, depth = P(F, T), P(T, F), P(T), P(F)
    placed = (
        rows, P(), wide, cols, wide, cols, tall, depth,
        wide, cols, wide, cols, wide, cols, tall, depth,
        P(), cols,
    )
    return jax.shard_map(on_device, mesh=fine, in_specs=placed, out_specs=rows, check_vma=False)
```

```python
import math

import jax
import jax.numpy as jnp
from jax import lax
from jax.experimental import pallas as pl
from jax.experimental.pallas import tpu as pltpu
from jax.sharding import Mesh, PartitionSpec as P


DK = 256
BLOCK = 64
EPSILON = 1e-05
NZ, NY, NX = 8, 4, 4
ROWS = 32
VMEM = pl.BlockSpec(memory_space=pltpu.VMEM)
SMEM = pl.BlockSpec(memory_space=pltpu.SMEM)
ANY = pl.BlockSpec(memory_space=pl.ANY)


def dot(a, b):
    return jnp.dot(a, b, preferred_element_type=jnp.float32)


def dot_t(a, b):
    return lax.dot_general(a, b, (((1,), (1,)), ((), ())), preferred_element_type=jnp.float32)


def low(w):
    return w.astype(jnp.bfloat16)


NEAR = (0, -1, 1, -2, 2)
DISTANT = (-3, 3, -4)
SIDES = (0, -1, 1, 2)
RING = (0, -1, -2, -3, -4, 1, 2, 3)


def plain(dz, dy):
    return dz % NZ * NY + dy % NY


FFN_ORDER = [plain(dz, dy) for dzs in (NEAR, DISTANT) for dy in SIDES for dz in dzs]
MIX_ORDER = [plain(dz, dy) for dz in RING for dy in range(NY)]
PLAIN_TO_FFN = FFN_ORDER
FFN_TO_PLAIN = [FFN_ORDER.index(b) for b in range(NZ * NY)]
FFN_TO_MIX = [FFN_ORDER.index(b) for b in MIX_ORDER]
MIX_TO_FFN = [MIX_ORDER.index(b) for b in FFN_ORDER]


def joined(tiles):
    (a, turn_a), (b, turn_b) = tiles
    lane = lax.broadcasted_iota(jnp.int32, a.shape, 1)
    a, b = (
        jnp.where(t, pltpu.roll(v, 64, 1), v) if not isinstance(t, bool) else (pltpu.roll(v, 64, 1) if t else v)
        for v, t in ((a, turn_a), (b, turn_b))
    )
    return jnp.where(lane < 64, a, b)


def shuffled(value, order):
    tiles = []
    for p, q in zip(order[::2], order[1::2]):
        a, b = (value[:, i // 2 * 128 : i // 2 * 128 + 128] for i in (p, q))
        tiles.append(joined(((a, p % 2 == 1), (b, q % 2 == 0))))
    return jnp.concatenate(tiles, axis=1)


def turned(ref, z, y):
    tiles = []
    for t in range(NZ * NY // 2):
        pair = []
        for half in range(2):
            b = 2 * t + half
            side = lax.rem(b % NY + y, NY)
            at = pl.multiple_of((lax.rem(b // NY + z, NZ) * (NY // 2) + side // 2) * 128, 128)
            pair.append((ref[:, pl.ds(at, 128)].astype(jnp.float32), side % 2 != half))
        tiles.append(joined(pair))
    return jnp.concatenate(tiles, axis=1)


def normed(stream, gain):
    scale = lax.rsqrt(jnp.mean(stream * stream, axis=-1, keepdims=True) + EPSILON)
    return low(stream * scale * gain)


def pack_kernel(place, gate, up, down, ds, query, key, value, out, os, tokens, gains, *rest):
    small, (ffn_ref, mix_ref, rows_ref, small_ref, stream_ref, gains_ref) = rest[:-6], rest[-6:]

    def column(row):
        n = row.shape[1]
        i = lax.broadcasted_iota(jnp.int32, (n, n), 0)
        j = lax.broadcasted_iota(jnp.int32, (n, n), 1)
        return jnp.sum(jnp.where(i == j, row, 0.0), axis=1, keepdims=True)

    def scaled(w, s):
        return low(low(w[...]).astype(jnp.float32) * column(s[...]))

    n = gate.shape[1]
    ffn_ref[:, :n] = low(gate[...])
    ffn_ref[:, n : 2 * n] = low(up[...])
    ffn_ref[:, 2 * n :] = scaled(down, ds)
    mix = (low(query[...]), low(key[...]), low(value[...]), scaled(out, os))
    for k in range(NY):
        for i, w in enumerate(mix):
            mix_ref[k, :, i * DK : (i + 1) * DK] = w
    z, y = place[0], place[1]
    stream = shuffled(turned(tokens, z, y), PLAIN_TO_FFN)
    ordered = shuffled(turned(gains, z, y), PLAIN_TO_FFN)
    stream_ref[...] = low(stream)
    gains_ref[...] = ordered
    first = normed(stream, ordered[:1, :])
    for k in range(rows_ref.shape[0]):
        rows_ref[k] = first
    for i, v in enumerate(small):
        small_ref[i : i + 1, : v.shape[1]] = v[...]


def pack(place, gate, up, down, ds, query, key, value, out, os, tokens, gains, small):
    rows, n = gate.shape
    return pl.pallas_call(
        pack_kernel,
        out_shape=(
            jax.ShapeDtypeStruct((rows, 3 * n), jnp.bfloat16),
            jax.ShapeDtypeStruct((NY, rows, 4 * DK), jnp.bfloat16),
            jax.ShapeDtypeStruct((2 * NX, *tokens.shape), jnp.bfloat16),
            jax.ShapeDtypeStruct((8, n), jnp.float32),
            jax.ShapeDtypeStruct(tokens.shape, jnp.bfloat16),
            jax.ShapeDtypeStruct(gains.shape, jnp.float32),
        ),
        in_specs=[SMEM] + [VMEM] * (11 + len(small)),
        out_specs=(VMEM,) * 6,
        compiler_params=pltpu.CompilerParams(vmem_limit_bytes=12 * 1024 * 1024),
        name="pack",
    )(place, gate, up, down, ds, query, key, value, out, os, tokens, gains, *small)


def join_kernel(weight, which, arrived_as, rows_as, place, arrived, stream, gains, next_ref, last_ref):
    total = arrived[0].astype(jnp.float32)
    for k in range(1, NX):
        total = total + arrived[k].astype(jnp.float32)
    if arrived_as is not None:
        total = shuffled(total, arrived_as)
    total = stream[...].astype(jnp.float32) + weight * total
    if which is None:
        z, y = place[0], place[1]
        last_ref[...] = shuffled(total, FFN_TO_PLAIN)
        next_ref[...] = low(turned(last_ref, NZ - z, NY - y))
        return
    next_ref[...] = total
    rows = total * lax.rsqrt(jnp.mean(total * total, axis=-1, keepdims=True) + EPSILON)
    rows = rows * gains[which : which + 1, :]
    if rows_as is not None:
        rows = shuffled(rows, rows_as)
    rows = low(rows)
    for k in range(NX):
        last_ref[k] = rows


def join(place, weight, which, arrived, stream, gains, arrived_as=None, rows_as=None):
    shape = stream.shape
    last = which is None
    outs = [jax.ShapeDtypeStruct(shape, jnp.bfloat16 if last else jnp.float32)]
    if not last:
        outs.append(jax.ShapeDtypeStruct((NX, *shape), jnp.bfloat16))
    return pl.pallas_call(
        lambda *refs: join_kernel(weight, which, arrived_as, rows_as, *refs),
        out_shape=outs,
        in_specs=[SMEM] + [VMEM] * 3,
        out_specs=[VMEM] * len(outs),
        scratch_shapes=[pltpu.VMEM(shape, jnp.float32)] if last else [],
        compiler_params=pltpu.CompilerParams(vmem_limit_bytes=8 * 1024 * 1024),
        name="join",
    )(place, arrived, stream, gains)


def along_z(array, step):
    return lax.ppermute(array, ("rep", "z"), [(g, (g + step) % (2 * NZ)) for g in range(2 * NZ)])


def along_y(array, step):
    return lax.ppermute(array, "y", [(g, (g + step) % NY) for g in range(NY)])


def gather_ffn(mine):
    u1, d1 = along_z(mine, 1), along_z(mine, -1)
    u2, d2 = along_z(u1, 1), along_z(d1, -1)
    u3, d3 = along_z(u1, 2), along_z(d1, -2)
    u4 = along_z(u2, 2)
    arrays = []

    def spread(blocks, far_up):
        own = jnp.stack(blocks)
        below = along_y(own, 1)
        above = along_y(own, -1)
        far = along_y(below, 1) if far_up else along_y(above, -1)
        arrays.extend((own, below, above, far))

    spread([mine, u1, d1, u2, d2], True)
    spread([u3, d3, u4], False)
    return arrays


def gather_mix(copies):
    mine = lax.all_to_all(copies, "y", split_axis=0, concat_axis=0, tiled=True)
    mine = lax.dynamic_slice_in_dim(jnp.concatenate([mine, mine]), lax.axis_index("y"), NY)
    mine = mine.reshape(-1, copies.shape[2])
    up, down = [mine], [mine]
    for k in range(4):
        up.append(along_z(up[-1], 1))
        if k < 3:
            down.append(along_z(down[-1], -1))
    return up + down[1:]


def swap_cores(array):
    return lax.ppermute(array, "core", [(0, 1), (1, 0)])


def gather_rows(copies):
    own = lax.all_to_all(copies, "x", split_axis=0, concat_axis=0, tiled=True)
    own = own.reshape(-1, copies.shape[2])
    return own, swap_cores(own)


def return_rows(own, other):
    swapped = swap_cores(other)
    both = low(own + swapped.astype(jnp.float32))
    blocks = both.reshape(NX, -1, both.shape[1])
    return lax.all_to_all(blocks, "x", split_axis=0, concat_axis=0, tiled=True)


def stacked(arrays, first, last):
    return jnp.concatenate([a[..., first:last].reshape(-1, last - first) for a in arrays], axis=0)


def ffn_kernel(spans, place, small, *rest):
    row_refs, arrays, (own_ref, other_ref) = rest[:spans], rest[spans:-2], rest[-2:]
    units = arrays[0].shape[-1] // 3
    core = place[2]
    if spans == 1:
        every = row_refs[0]
        sides = [core, 1 - core]
        rows = jnp.concatenate([every[2 * k + s] for s in sides for k in range(NX)], axis=0)
    else:
        rows = jnp.concatenate([r[...] for r in row_refs], axis=0)
    gate = dot(rows, stacked(arrays, 0, units)) * small[0:1, :]
    up = dot(rows, stacked(arrays, units, 2 * units)) * small[1:2, :]
    hidden = low(gate / (1.0 + jnp.exp(-gate)) * up)
    part = dot_t(hidden, stacked(arrays, 2 * units, 3 * units))
    half = own_ref.shape[0]
    own_ref[...] = part[:half]
    other_ref[...] = low(part[half:])


def feed_forward(place, small, row_arrays, arrays):
    wide = row_arrays[0].shape[-1]
    rows = NX * ROWS
    own_part, other_part = pl.pallas_call(
        lambda *refs: ffn_kernel(len(row_arrays), *refs),
        out_shape=(
            jax.ShapeDtypeStruct((rows, wide), jnp.float32),
            jax.ShapeDtypeStruct((rows, wide), jnp.bfloat16),
        ),
        in_specs=[SMEM, VMEM] + [VMEM] * len(row_arrays) + [VMEM] * len(arrays),
        out_specs=(VMEM, VMEM),
        compiler_params=pltpu.CompilerParams(vmem_limit_bytes=24 * 1024 * 1024),
        name="ffn",
    )(place, small, *row_arrays, *arrays)
    return return_rows(own_part, other_part)


def mix_kernel(place, rate, small, own_rows, other_rows, *rest):
    arrays, (own_ref, other_ref) = rest[:-2], rest[-2:]
    core = place[2]
    rows = jnp.concatenate([own_rows[...], other_rows[...]], axis=0)
    query = low(dot(rows, stacked(arrays, 0, DK)) * small[2:3, :DK])
    key_rows = low(dot(rows, stacked(arrays, DK, 2 * DK)) * small[3:4, :DK] / math.sqrt(DK))
    value = low(dot(rows, stacked(arrays, 2 * DK, 3 * DK)) * small[4:5, :DK])

    total = rows.shape[0]

    def position(axis):
        r = lax.broadcasted_iota(jnp.int32, (total, total), axis)
        half = r // (total // 2)
        side = jnp.where(half == 0, core, 1 - core)
        return (r % (total // 2)) // ROWS * (2 * ROWS) + side * ROWS + r % ROWS

    pi, pj = position(0), position(1)
    apart = jnp.abs(pi - pj).astype(jnp.float32)
    decay = jnp.where(pj // BLOCK <= pi // BLOCK, jnp.exp(-rate[0] * apart), 0.0)
    scores = low(dot_t(query, key_rows) * decay)
    retained = dot(scores, value)
    centred = retained - jnp.mean(retained, axis=-1, keepdims=True)
    scale = lax.rsqrt(jnp.mean(centred * centred, axis=-1, keepdims=True) + EPSILON)
    mixed = low(centred * scale * small[5:6, :DK])
    part = dot_t(mixed, stacked(arrays, 3 * DK, 4 * DK))
    half = own_ref.shape[0]
    own_ref[...] = part[:half]
    other_ref[...] = low(part[half:])


def mix(place, rate, small, own, other, arrays):
    rows, wide = own.shape
    own_part, other_part = pl.pallas_call(
        mix_kernel,
        out_shape=(
            jax.ShapeDtypeStruct((rows, wide), jnp.float32),
            jax.ShapeDtypeStruct((rows, wide), jnp.bfloat16),
        ),
        in_specs=[SMEM, SMEM] + [VMEM] * (3 + len(arrays)),
        out_specs=(VMEM, VMEM),
        compiler_params=pltpu.CompilerParams(vmem_limit_bytes=24 * 1024 * 1024),
        name="mix",
    )(place, rate, small, own, other, *arrays)
    return return_rows(own_part, other_part)


def on_device(
    tokens_in, norm_gains, gate_w, gate_scale, up_w, up_scale, down_w, down_scale,
    query_w, query_scale, key_w, key_scale, value_w, value_scale, out_w, out_scale,
    head_gain, decay_rate,
):
    def row(v):
        return v.reshape(1, -1)

    place = jnp.stack([lax.axis_index(a).astype(jnp.int32) for a in ("z", "y", "core")])
    ffn_mine, mix_mine, copies, small, stream, gains = pack(
        place, gate_w, up_w, down_w.T, row(down_scale), query_w, key_w, value_w, out_w.T,
        row(out_scale), tokens_in, norm_gains,
        [row(v) for v in (gate_scale, up_scale, query_scale, key_scale, value_scale, head_gain)],
    )
    ffn_arrays = gather_ffn(ffn_mine)
    every = lax.all_to_all(copies, ("x", "core"), split_axis=0, concat_axis=0, tiled=True)
    mix_arrays = gather_mix(mix_mine)

    arrived = feed_forward(place, small, [every], ffn_arrays)
    stream, copies = join(place, 0.5, 1, arrived, stream, gains, rows_as=FFN_TO_MIX)
    own, other = gather_rows(copies)
    arrived = mix(place, decay_rate, small, own, other, mix_arrays)
    stream, copies = join(place, 1.0, 2, arrived, stream, gains, arrived_as=MIX_TO_FFN)
    rows = gather_rows(copies)
    arrived = feed_forward(place, small, rows, ffn_arrays)
    return join(place, 0.5, None, arrived, stream, gains)[0]


def solution(mesh):
    devices = mesh.devices
    fine = Mesh(devices.reshape(2, NZ, NY, NX, 2), ("rep", "z", "y", "x", "core"))
    F, T = ("z", "y"), ("x", "core")
    rows = P(("rep", "z", "y", "x", "core"), None)
    wide, tall, cols, depth = P(F, T), P(T, F), P(T), P(F)
    placed = (
        rows, P(), wide, cols, wide, cols, tall, depth,
        wide, cols, wide, cols, wide, cols, tall, depth,
        P(), cols,
    )
    return jax.shard_map(on_device, mesh=fine, in_specs=placed, out_specs=rows, check_vma=False)
```

```python
import math

import jax
import jax.numpy as jnp
from jax import lax
from jax.experimental import pallas as pl
from jax.experimental.pallas import tpu as pltpu
from jax.sharding import Mesh, PartitionSpec as P


DK = 256
BLOCK = 64
EPSILON = 1e-05
NZ, NY, NX = 8, 4, 4
ROWS = 32
VMEM = pl.BlockSpec(memory_space=pltpu.VMEM)
SMEM = pl.BlockSpec(memory_space=pltpu.SMEM)
ANY = pl.BlockSpec(memory_space=pl.ANY)


def dot(a, b):
    return jnp.dot(a, b, preferred_element_type=jnp.float32)


def dot_t(a, b):
    return lax.dot_general(a, b, (((1,), (1,)), ((), ())), preferred_element_type=jnp.float32)


def low(w):
    return w.astype(jnp.bfloat16)


NEAR = (0, -1, 1, -2, 2)
DISTANT = (-3, 3, -4)
SIDES = (0, -1, 1, 2)
RING = (0, -1, -2, -3, -4, 1, 2, 3)


def plain(dz, dy):
    return dz % NZ * NY + dy % NY


FFN_ORDER = [plain(dz, dy) for dzs in (NEAR, DISTANT) for dy in SIDES for dz in dzs]
MIX_ORDER = [plain(dz, dy) for dz in RING for dy in range(NY)]
PLAIN_TO_FFN = FFN_ORDER
FFN_TO_PLAIN = [FFN_ORDER.index(b) for b in range(NZ * NY)]
FFN_TO_MIX = [FFN_ORDER.index(b) for b in MIX_ORDER]
MIX_TO_FFN = [MIX_ORDER.index(b) for b in FFN_ORDER]


def joined(tiles):
    (a, turn_a), (b, turn_b) = tiles
    lane = lax.broadcasted_iota(jnp.int32, a.shape, 1)
    a, b = (
        jnp.where(t, pltpu.roll(v, 64, 1), v) if not isinstance(t, bool) else (pltpu.roll(v, 64, 1) if t else v)
        for v, t in ((a, turn_a), (b, turn_b))
    )
    return jnp.where(lane < 64, a, b)


def shuffled(value, order):
    tiles = []
    for p, q in zip(order[::2], order[1::2]):
        a, b = (value[:, i // 2 * 128 : i // 2 * 128 + 128] for i in (p, q))
        tiles.append(joined(((a, p % 2 == 1), (b, q % 2 == 0))))
    return jnp.concatenate(tiles, axis=1)


def turned_in_place(value, y):
    wide = 64 * NY
    shift = lax.rem(wide - 64 * y, wide)
    groups = [value[:, g : g + wide] for g in range(0, value.shape[1], wide)]
    return jnp.concatenate([pltpu.roll(g, shift, 1) for g in groups], axis=1)


def turned(ref, z, y):
    tiles = []
    for t in range(NZ * NY // 2):
        pair = []
        for half in range(2):
            b = 2 * t + half
            side = lax.rem(b % NY + y, NY)
            at = pl.multiple_of((lax.rem(b // NY + z, NZ) * (NY // 2) + side // 2) * 128, 128)
            pair.append((ref[:, pl.ds(at, 128)].astype(jnp.float32), side % 2 != half))
        tiles.append(joined(pair))
    return jnp.concatenate(tiles, axis=1)


def normed(stream, gain):
    scale = lax.rsqrt(jnp.mean(stream * stream, axis=-1, keepdims=True) + EPSILON)
    return low(stream * scale * gain)


def pack_kernel(place, gate, up, down, ds, query, key, value, out, os, tokens, gains, *rest):
    small, (ffn_ref, mix_ref, rows_ref, small_ref, stream_ref, gains_ref) = rest[:-6], rest[-6:]

    def column(row):
        n = row.shape[1]
        i = lax.broadcasted_iota(jnp.int32, (n, n), 0)
        j = lax.broadcasted_iota(jnp.int32, (n, n), 1)
        return jnp.sum(jnp.where(i == j, row, 0.0), axis=1, keepdims=True)

    def scaled(w, s):
        return low(low(w[...]).astype(jnp.float32) * column(s[...]))

    n = gate.shape[1]
    ffn_ref[:, :n] = low(gate[...])
    ffn_ref[:, n : 2 * n] = low(up[...])
    ffn_ref[:, 2 * n :] = scaled(down, ds)
    mix = (low(query[...]), low(key[...]), low(value[...]), scaled(out, os))
    for k in range(NY):
        for i, w in enumerate(mix):
            mix_ref[k, :, i * DK : (i + 1) * DK] = w
    z, y = place[0], place[1]
    stream = shuffled(turned(tokens, z, y), PLAIN_TO_FFN)
    ordered = shuffled(turned(gains, z, y), PLAIN_TO_FFN)
    stream_ref[...] = low(stream)
    gains_ref[...] = ordered
    first = normed(stream, ordered[:1, :])
    for k in range(rows_ref.shape[0]):
        rows_ref[k] = first
    for i, v in enumerate(small):
        for k in range(v.shape[0]):
            small_ref[i : i + 1, k * 128 : k * 128 + 128] = v[k : k + 1, :]


def pack(place, gate, up, down, ds, query, key, value, out, os, tokens, gains, small):
    rows, n = gate.shape
    return pl.pallas_call(
        pack_kernel,
        out_shape=(
            jax.ShapeDtypeStruct((rows, 3 * n), jnp.bfloat16),
            jax.ShapeDtypeStruct((NY, rows, 4 * DK), jnp.bfloat16),
            jax.ShapeDtypeStruct((2 * NX, *tokens.shape), jnp.bfloat16),
            jax.ShapeDtypeStruct((8, n), jnp.float32),
            jax.ShapeDtypeStruct(tokens.shape, jnp.bfloat16),
            jax.ShapeDtypeStruct(gains.shape, jnp.float32),
        ),
        in_specs=[SMEM] + [VMEM] * (11 + len(small)),
        out_specs=(VMEM,) * 6,
        name="pack",
    )(place, gate, up, down, ds, query, key, value, out, os, tokens, gains, *small)


def join_kernel(weight, which, arrived_as, rows_as, place, arrived, stream, gains, next_ref, last_ref):
    total = arrived[0].astype(jnp.float32)
    for k in range(1, NX):
        total = total + arrived[k].astype(jnp.float32)
    if arrived_as is not None:
        total = shuffled(turned_in_place(total, place[1]), arrived_as)
    total = stream[...].astype(jnp.float32) + weight * total
    if which is None:
        z, y = place[0], place[1]
        last_ref[...] = shuffled(total, FFN_TO_PLAIN)
        next_ref[...] = low(turned(last_ref, NZ - z, NY - y))
        return
    next_ref[...] = total
    rows = total * lax.rsqrt(jnp.mean(total * total, axis=-1, keepdims=True) + EPSILON)
    rows = rows * gains[which : which + 1, :]
    if rows_as is not None:
        rows = turned_in_place(shuffled(rows, rows_as), NY - place[1])
    rows = low(rows)
    for k in range(NX):
        last_ref[k] = rows


def join(place, weight, which, arrived, stream, gains, arrived_as=None, rows_as=None):
    shape = stream.shape
    last = which is None
    outs = [jax.ShapeDtypeStruct(shape, jnp.bfloat16 if last else jnp.float32)]
    if not last:
        outs.append(jax.ShapeDtypeStruct((NX, *shape), jnp.bfloat16))
    return pl.pallas_call(
        lambda *refs: join_kernel(weight, which, arrived_as, rows_as, *refs),
        out_shape=outs,
        in_specs=[SMEM] + [VMEM] * 3,
        out_specs=[VMEM] * len(outs),
        scratch_shapes=[pltpu.VMEM(shape, jnp.float32)] if last else [],
        compiler_params=pltpu.CompilerParams(vmem_limit_bytes=8 * 1024 * 1024),
        name="join",
    )(place, arrived, stream, gains)


def along_z(array, step):
    return lax.ppermute(array, ("rep", "z"), [(g, (g + step) % (2 * NZ)) for g in range(2 * NZ)])


def along_y(array, step):
    return lax.ppermute(array, "y", [(g, (g + step) % NY) for g in range(NY)])


def gather_ffn(mine):
    u1, d1 = along_z(mine, 1), along_z(mine, -1)
    u2, d2 = along_z(u1, 1), along_z(d1, -1)
    u3, d3 = along_z(u1, 2), along_z(d1, -2)
    u4 = along_z(u2, 2)
    arrays = []

    def spread(blocks, far_up):
        own = jnp.stack(blocks)
        below = along_y(own, 1)
        above = along_y(own, -1)
        far = along_y(below, 1) if far_up else along_y(above, -1)
        arrays.extend((own, below, above, far))

    spread([mine, u1, d1, u2, d2], True)
    spread([u3, d3, u4], False)
    return arrays


def gather_mix(copies):
    mine = lax.all_to_all(copies, "y", split_axis=0, concat_axis=0, tiled=True)
    mine = mine.reshape(-1, copies.shape[2])
    up, down = [mine], [mine]
    for k in range(4):
        up.append(along_z(up[-1], 1))
        if k < 3:
            down.append(along_z(down[-1], -1))
    return up + down[1:]


def swap_cores(array):
    return lax.ppermute(array, "core", [(0, 1), (1, 0)])


def gather_rows(copies):
    own = lax.all_to_all(copies, "x", split_axis=0, concat_axis=0, tiled=True)
    own = own.reshape(-1, copies.shape[2])
    return own, swap_cores(own)


def return_rows(own, other):
    swapped = swap_cores(other)
    both = low(own + swapped.astype(jnp.float32))
    blocks = both.reshape(NX, -1, both.shape[1])
    return lax.all_to_all(blocks, "x", split_axis=0, concat_axis=0, tiled=True)


def stacked(arrays, first, last):
    return jnp.concatenate([a[..., first:last].reshape(-1, last - first) for a in arrays], axis=0)


def ffn_kernel(spans, place, small, *rest):
    row_refs, arrays, (own_ref, other_ref) = rest[:spans], rest[spans:-2], rest[-2:]
    units = arrays[0].shape[-1] // 3
    core = place[2]
    if spans == 1:
        every = row_refs[0]
        sides = [core, 1 - core]
        rows = jnp.concatenate([every[2 * k + s] for s in sides for k in range(NX)], axis=0)
    else:
        rows = jnp.concatenate([r[...] for r in row_refs], axis=0)
    gate = dot(rows, stacked(arrays, 0, units)) * small[0:1, :]
    up = dot(rows, stacked(arrays, units, 2 * units)) * small[1:2, :]
    hidden = low(gate / (1.0 + jnp.exp(-gate)) * up)
    part = dot_t(hidden, stacked(arrays, 2 * units, 3 * units))
    half = own_ref.shape[0]
    own_ref[...] = part[:half]
    other_ref[...] = low(part[half:])


def feed_forward(place, small, row_arrays, arrays):
    wide = row_arrays[0].shape[-1]
    rows = NX * ROWS
    own_part, other_part = pl.pallas_call(
        lambda *refs: ffn_kernel(len(row_arrays), *refs),
        out_shape=(
            jax.ShapeDtypeStruct((rows, wide), jnp.float32),
            jax.ShapeDtypeStruct((rows, wide), jnp.bfloat16),
        ),
        in_specs=[SMEM, VMEM] + [VMEM] * len(row_arrays) + [VMEM] * len(arrays),
        out_specs=(VMEM, VMEM),
        compiler_params=pltpu.CompilerParams(vmem_limit_bytes=24 * 1024 * 1024),
        name="ffn",
    )(place, small, *row_arrays, *arrays)
    return return_rows(own_part, other_part)


def mix_kernel(place, rate, small, own_rows, other_rows, *rest):
    arrays, (own_ref, other_ref) = rest[:-2], rest[-2:]
    core = place[2]
    rows = jnp.concatenate([own_rows[...], other_rows[...]], axis=0)
    query = low(dot(rows, stacked(arrays, 0, DK)) * small[2:3, :DK])
    key_rows = low(dot(rows, stacked(arrays, DK, 2 * DK)) * small[3:4, :DK] / math.sqrt(DK))
    value = low(dot(rows, stacked(arrays, 2 * DK, 3 * DK)) * small[4:5, :DK])

    total = rows.shape[0]

    def position(axis):
        r = lax.broadcasted_iota(jnp.int32, (total, total), axis)
        half = r // (total // 2)
        side = jnp.where(half == 0, core, 1 - core)
        return (r % (total // 2)) // ROWS * (2 * ROWS) + side * ROWS + r % ROWS

    pi, pj = position(0), position(1)
    apart = jnp.abs(pi - pj).astype(jnp.float32)
    decay = jnp.where(pj // BLOCK <= pi // BLOCK, jnp.exp(-rate[0] * apart), 0.0)
    scores = low(dot_t(query, key_rows) * decay)
    retained = dot(scores, value)
    centred = retained - jnp.mean(retained, axis=-1, keepdims=True)
    scale = lax.rsqrt(jnp.mean(centred * centred, axis=-1, keepdims=True) + EPSILON)
    mixed = low(centred * scale * small[5:6, :DK])
    part = dot_t(mixed, stacked(arrays, 3 * DK, 4 * DK))
    half = own_ref.shape[0]
    own_ref[...] = part[:half]
    other_ref[...] = low(part[half:])


def mix(place, rate, small, own, other, arrays):
    rows, wide = own.shape
    own_part, other_part = pl.pallas_call(
        mix_kernel,
        out_shape=(
            jax.ShapeDtypeStruct((rows, wide), jnp.float32),
            jax.ShapeDtypeStruct((rows, wide), jnp.bfloat16),
        ),
        in_specs=[SMEM, SMEM] + [VMEM] * (3 + len(arrays)),
        out_specs=(VMEM, VMEM),
        compiler_params=pltpu.CompilerParams(vmem_limit_bytes=24 * 1024 * 1024),
        name="mix",
    )(place, rate, small, own, other, *arrays)
    return return_rows(own_part, other_part)


def on_device(
    tokens_in, norm_gains, gate_w, gate_scale, up_w, up_scale, down_w, down_scale,
    query_w, query_scale, key_w, key_scale, value_w, value_scale, out_w, out_scale,
    head_gain, decay_rate,
):
    def row(v):
        return v.reshape(1, -1)

    place = jnp.stack([lax.axis_index(a).astype(jnp.int32) for a in ("z", "y", "core")])
    ffn_mine, mix_mine, copies, small, stream, gains = pack(
        place, gate_w, up_w, down_w.T, row(down_scale), query_w, key_w, value_w, out_w.T,
        row(out_scale), tokens_in, norm_gains,
        [v.reshape(-1, 128) for v in (gate_scale, up_scale, query_scale, key_scale, value_scale, head_gain)],
    )
    ffn_arrays = gather_ffn(ffn_mine)
    every = lax.all_to_all(copies, ("x", "core"), split_axis=0, concat_axis=0, tiled=True)
    mix_arrays = gather_mix(mix_mine)

    arrived = feed_forward(place, small, [every], ffn_arrays)
    stream, copies = join(place, 0.5, 1, arrived, stream, gains, rows_as=FFN_TO_MIX)
    own, other = gather_rows(copies)
    arrived = mix(place, decay_rate, small, own, other, mix_arrays)
    stream, copies = join(place, 1.0, 2, arrived, stream, gains, arrived_as=MIX_TO_FFN)
    rows = gather_rows(copies)
    arrived = feed_forward(place, small, rows, ffn_arrays)
    return join(place, 0.5, None, arrived, stream, gains)[0]


def solution(mesh):
    devices = mesh.devices
    fine = Mesh(devices.reshape(2, NZ, NY, NX, 2), ("rep", "z", "y", "x", "core"))
    F, T = ("z", "y"), ("x", "core")
    rows = P(("rep", "z", "y", "x", "core"), None)
    wide, tall, cols, depth = P(F, T), P(T, F), P(T), P(F)
    placed = (
        rows, P(), wide, cols, wide, cols, tall, depth,
        wide, cols, wide, cols, wide, cols, tall, depth,
        P(), cols,
    )
    return jax.shard_map(on_device, mesh=fine, in_specs=placed, out_specs=rows, check_vma=False)
```

```python
import math

import jax
import jax.numpy as jnp
from jax import lax
from jax.experimental import pallas as pl
from jax.experimental.pallas import tpu as pltpu
from jax.sharding import Mesh, PartitionSpec as P


DK = 256
BLOCK = 64
EPSILON = 1e-05
NZ, NY, NX = 8, 4, 4
ROWS = 32
VMEM = pl.BlockSpec(memory_space=pltpu.VMEM)


def dot(a, b):
    return jnp.dot(a, b, preferred_element_type=jnp.float32)


def dot_t(a, b):
    return lax.dot_general(a, b, (((1,), (1,)), ((), ())), preferred_element_type=jnp.float32)


def low(w):
    return w.astype(jnp.bfloat16)


NEAR = (0, -1, 1, -2, 2)
DISTANT = (-3, 3, -4)
SIDES = (0, -1, 1, 2)
RING = (0, -1, -2, -3, -4, 1, 2, 3)


def plain(dz, dy):
    return dz % NZ * NY + dy % NY


FFN_ORDER = [plain(dz, dy) for dzs in (NEAR, DISTANT) for dy in SIDES for dz in dzs]
MIX_ORDER = [plain(dz, dy) for dz in RING for dy in range(NY)]
PLAIN_TO_FFN = FFN_ORDER
FFN_TO_PLAIN = [FFN_ORDER.index(b) for b in range(NZ * NY)]
FFN_TO_MIX = [FFN_ORDER.index(b) for b in MIX_ORDER]
MIX_TO_FFN = [MIX_ORDER.index(b) for b in FFN_ORDER]


def joined(tiles):
    (a, turn_a), (b, turn_b) = tiles
    lane = lax.broadcasted_iota(jnp.int32, a.shape, 1)
    a, b = (
        jnp.where(t, pltpu.roll(v, 64, 1), v) if not isinstance(t, bool) else (pltpu.roll(v, 64, 1) if t else v)
        for v, t in ((a, turn_a), (b, turn_b))
    )
    return jnp.where(lane < 64, a, b)


def shuffled(value, order):
    tiles = []
    for p, q in zip(order[::2], order[1::2]):
        a, b = (value[:, i // 2 * 128 : i // 2 * 128 + 128] for i in (p, q))
        tiles.append(joined(((a, p % 2 == 1), (b, q % 2 == 0))))
    return jnp.concatenate(tiles, axis=1)


def turned_in_place(value, y):
    wide = 64 * NY
    shift = lax.rem(wide - 64 * y, wide)
    groups = [value[:, g : g + wide] for g in range(0, value.shape[1], wide)]
    return jnp.concatenate([pltpu.roll(g, shift, 1) for g in groups], axis=1)


def turned(ref, z, y):
    tiles = []
    for t in range(NZ * NY // 2):
        pair = []
        for half in range(2):
            b = 2 * t + half
            side = lax.rem(b % NY + y, NY)
            at = pl.multiple_of((lax.rem(b // NY + z, NZ) * (NY // 2) + side // 2) * 128, 128)
            pair.append((ref[:, pl.ds(at, 128)].astype(jnp.float32), side % 2 != half))
        tiles.append(joined(pair))
    return jnp.concatenate(tiles, axis=1)


def normed(stream, gain):
    scale = lax.rsqrt(jnp.mean(stream * stream, axis=-1, keepdims=True) + EPSILON)
    return low(stream * scale * gain)


def pack_kernel(gate, up, down, ds, query, key, value, out, os, tokens, gains, *rest):
    small, (ffn_ref, mix_ref, rows_ref, small_ref, stream_ref, gains_ref) = rest[:-6], rest[-6:]

    def column(row):
        n = row.shape[1]
        i = lax.broadcasted_iota(jnp.int32, (n, n), 0)
        j = lax.broadcasted_iota(jnp.int32, (n, n), 1)
        return jnp.sum(jnp.where(i == j, row, 0.0), axis=1, keepdims=True)

    def scaled(w, s):
        return low(low(w[...]).astype(jnp.float32) * column(s[...]))

    n = gate.shape[1]
    ffn_ref[:, :n] = low(gate[...])
    ffn_ref[:, n : 2 * n] = low(up[...])
    ffn_ref[:, 2 * n :] = scaled(down, ds)
    mix = (low(query[...]), low(key[...]), low(value[...]), scaled(out, os))
    for k in range(NY):
        for i, w in enumerate(mix):
            mix_ref[k, :, i * DK : (i + 1) * DK] = w
    z, y = lax.axis_index("z"), lax.axis_index("y")
    stream = shuffled(turned(tokens, z, y), PLAIN_TO_FFN)
    ordered = shuffled(turned(gains, z, y), PLAIN_TO_FFN)
    stream_ref[...] = low(stream)
    gains_ref[...] = ordered
    first = normed(stream, ordered[:1, :])
    for k in range(rows_ref.shape[0]):
        rows_ref[k] = first
    for i, v in enumerate(small):
        for k in range(v.shape[0]):
            row = jnp.broadcast_to(v[k : k + 1, :], (1, 128))
            small_ref[i : i + 1, k * 128 : k * 128 + 128] = row


def pack(gate, up, down, ds, query, key, value, out, os, tokens, gains, small):
    rows, n = gate.shape
    return pl.pallas_call(
        pack_kernel,
        out_shape=(
            jax.ShapeDtypeStruct((rows, 3 * n), jnp.bfloat16),
            jax.ShapeDtypeStruct((NY, rows, 4 * DK), jnp.bfloat16),
            jax.ShapeDtypeStruct((2 * NX, *tokens.shape), jnp.bfloat16),
            jax.ShapeDtypeStruct((8, n), jnp.float32),
            jax.ShapeDtypeStruct(tokens.shape, jnp.bfloat16),
            jax.ShapeDtypeStruct(gains.shape, jnp.float32),
        ),
        in_specs=[VMEM] * (11 + len(small)),
        out_specs=(VMEM,) * 6,
        name="pack",
    )(gate, up, down, ds, query, key, value, out, os, tokens, gains, *small)


def join_kernel(weight, which, arrived_as, rows_as, arrived, stream, gains, next_ref, last_ref):
    total = arrived[0].astype(jnp.float32)
    for k in range(1, NX):
        total = total + arrived[k].astype(jnp.float32)
    if arrived_as is not None:
        total = shuffled(turned_in_place(total, lax.axis_index("y")), arrived_as)
    total = stream[...].astype(jnp.float32) + weight * total
    if which is None:
        z, y = lax.axis_index("z"), lax.axis_index("y")
        last_ref[...] = shuffled(total, FFN_TO_PLAIN)
        next_ref[...] = low(turned(last_ref, NZ - z, NY - y))
        return
    next_ref[...] = total
    rows = total * lax.rsqrt(jnp.mean(total * total, axis=-1, keepdims=True) + EPSILON)
    rows = rows * gains[which : which + 1, :]
    if rows_as is not None:
        rows = turned_in_place(shuffled(rows, rows_as), NY - lax.axis_index("y"))
    rows = low(rows)
    for k in range(NX):
        last_ref[k] = rows


def join(weight, which, arrived, stream, gains, arrived_as=None, rows_as=None):
    shape = stream.shape
    last = which is None
    outs = [jax.ShapeDtypeStruct(shape, jnp.bfloat16 if last else jnp.float32)]
    if not last:
        outs.append(jax.ShapeDtypeStruct((NX, *shape), jnp.bfloat16))
    return pl.pallas_call(
        lambda *refs: join_kernel(weight, which, arrived_as, rows_as, *refs),
        out_shape=outs,
        in_specs=[VMEM] * 3,
        out_specs=[VMEM] * len(outs),
        scratch_shapes=[pltpu.VMEM(shape, jnp.float32)] if last else [],
        compiler_params=pltpu.CompilerParams(vmem_limit_bytes=8 * 1024 * 1024),
        name="join",
    )(arrived, stream, gains)


def along_z(array, step):
    return lax.ppermute(array, ("rep", "z"), [(g, (g + step) % (2 * NZ)) for g in range(2 * NZ)])


def along_y(array, step):
    return lax.ppermute(array, "y", [(g, (g + step) % NY) for g in range(NY)])


def gather_ffn(mine):
    u1, d1 = along_z(mine, 1), along_z(mine, -1)
    u2, d2 = along_z(u1, 1), along_z(d1, -1)
    u3, d3 = along_z(u1, 2), along_z(d1, -2)
    u4 = along_z(u2, 2)
    arrays = []

    def spread(blocks, far_up):
        own = jnp.stack(blocks)
        below = along_y(own, 1)
        above = along_y(own, -1)
        far = along_y(below, 1) if far_up else along_y(above, -1)
        arrays.extend((own, below, above, far))

    spread([mine, u1, d1, u2, d2], True)
    spread([u3, d3, u4], False)
    return arrays


def pick_kernel(first, second, out):
    @pl.when(lax.axis_index("core") == 0)
    def _():
        out[...] = first[...]

    @pl.when(lax.axis_index("core") != 0)
    def _():
        out[...] = second[...]


def gather_mix(copies):
    mine = lax.all_to_all(copies, "y", split_axis=0, concat_axis=0, tiled=True)
    mine = mine.reshape(-1, copies.shape[2])

    u1, d1 = along_z(mine, 1), along_z(mine, -1)
    u2, d2 = along_z(u1, 1), along_z(d1, -1)
    d3, u3 = along_z(d1, -2), along_z(u2, 1)
    last = pl.pallas_call(
        pick_kernel,
        out_shape=jax.ShapeDtypeStruct(mine.shape, mine.dtype),
        in_specs=[VMEM, VMEM],
        out_specs=VMEM,
        compiler_params=pltpu.CompilerParams(vmem_limit_bytes=4 * 1024 * 1024),
        name="pick",
    )(u3, d3)
    ring = 2 * NZ
    pairs = [(2 * g + c, 2 * ((g + 1 - 2 * c) % ring) + c) for g in range(ring) for c in (0, 1)]
    last = lax.ppermute(last, ("rep", "z", "core"), pairs)
    return [mine, u1, u2, u3, last, d1, d2, d3]


def swap_cores(array):
    return lax.ppermute(array, "core", [(0, 1), (1, 0)])


def gather_rows(copies):
    own = lax.all_to_all(copies, "x", split_axis=0, concat_axis=0, tiled=True)
    own = own.reshape(-1, copies.shape[2])
    return own, swap_cores(own)


def return_rows(own, other):
    swapped = swap_cores(other)
    both = low(own + swapped.astype(jnp.float32))
    blocks = both.reshape(NX, -1, both.shape[1])
    return lax.all_to_all(blocks, "x", split_axis=0, concat_axis=0, tiled=True)


def stacked(arrays, first, last):
    return jnp.concatenate([a[..., first:last].reshape(-1, last - first) for a in arrays], axis=0)


def ffn_kernel(spans, small, *rest):
    row_refs, arrays, (own_ref, other_ref) = rest[:spans], rest[spans:-2], rest[-2:]
    units = arrays[0].shape[-1] // 3
    core = lax.axis_index("core")
    if spans == 1:
        every = row_refs[0]
        sides = [core, 1 - core]
        rows = jnp.concatenate([every[2 * k + s] for s in sides for k in range(NX)], axis=0)
    else:
        rows = jnp.concatenate([r[...] for r in row_refs], axis=0)
    gate = dot(rows, stacked(arrays, 0, units)) * small[0:1, :]
    up = dot(rows, stacked(arrays, units, 2 * units)) * small[1:2, :]
    hidden = low(gate / (1.0 + jnp.exp(-gate)) * up)
    part = dot_t(hidden, stacked(arrays, 2 * units, 3 * units))
    half = own_ref.shape[0]
    own_ref[...] = part[:half]
    other_ref[...] = low(part[half:])


def feed_forward(small, row_arrays, arrays):
    wide = row_arrays[0].shape[-1]
    rows = NX * ROWS
    own_part, other_part = pl.pallas_call(
        lambda *refs: ffn_kernel(len(row_arrays), *refs),
        out_shape=(
            jax.ShapeDtypeStruct((rows, wide), jnp.float32),
            jax.ShapeDtypeStruct((rows, wide), jnp.bfloat16),
        ),
        in_specs=[VMEM] + [VMEM] * len(row_arrays) + [VMEM] * len(arrays),
        out_specs=(VMEM, VMEM),
        compiler_params=pltpu.CompilerParams(vmem_limit_bytes=24 * 1024 * 1024),
        name="ffn",
    )(small, *row_arrays, *arrays)
    return return_rows(own_part, other_part)


def mix_kernel(small, own_rows, other_rows, *rest):
    arrays, (own_ref, other_ref) = rest[:-2], rest[-2:]
    core = lax.axis_index("core")
    rows = jnp.concatenate([own_rows[...], other_rows[...]], axis=0)
    query = low(dot(rows, stacked(arrays, 0, DK)) * small[2:3, :DK])
    key_rows = low(dot(rows, stacked(arrays, DK, 2 * DK)) * small[3:4, :DK] / math.sqrt(DK))
    value = low(dot(rows, stacked(arrays, 2 * DK, 3 * DK)) * small[4:5, :DK])

    total = rows.shape[0]

    def position(axis):
        r = lax.broadcasted_iota(jnp.int32, (total, total), axis)
        half = r // (total // 2)
        side = jnp.where(half == 0, core, 1 - core)
        return (r % (total // 2)) // ROWS * (2 * ROWS) + side * ROWS + r % ROWS

    pi, pj = position(0), position(1)
    apart = jnp.abs(pi - pj).astype(jnp.float32)
    decay = jnp.where(pj // BLOCK <= pi // BLOCK, jnp.exp(-small[6:7, :1] * apart), 0.0)
    scores = low(dot_t(query, key_rows) * decay)
    retained = dot(scores, value)
    centred = retained - jnp.mean(retained, axis=-1, keepdims=True)
    scale = lax.rsqrt(jnp.mean(centred * centred, axis=-1, keepdims=True) + EPSILON)
    mixed = low(centred * scale * small[5:6, :DK])
    part = dot_t(mixed, stacked(arrays, 3 * DK, 4 * DK))
    half = own_ref.shape[0]
    own_ref[...] = part[:half]
    other_ref[...] = low(part[half:])


def mix(small, own, other, arrays):
    rows, wide = own.shape
    own_part, other_part = pl.pallas_call(
        mix_kernel,
        out_shape=(
            jax.ShapeDtypeStruct((rows, wide), jnp.float32),
            jax.ShapeDtypeStruct((rows, wide), jnp.bfloat16),
        ),
        in_specs=[VMEM] * (3 + len(arrays)),
        out_specs=(VMEM, VMEM),
        compiler_params=pltpu.CompilerParams(vmem_limit_bytes=24 * 1024 * 1024),
        name="mix",
    )(small, own, other, *arrays)
    return return_rows(own_part, other_part)


def on_device(
    tokens_in, norm_gains, gate_w, gate_scale, up_w, up_scale, down_w, down_scale,
    query_w, query_scale, key_w, key_scale, value_w, value_scale, out_w, out_scale,
    head_gain, decay_rate,
):
    def row(v):
        return v.reshape(1, -1)

    ffn_mine, mix_mine, copies, small, stream, gains = pack(
        gate_w, up_w, down_w.T, row(down_scale), query_w, key_w, value_w, out_w.T,
        row(out_scale), tokens_in, norm_gains,
        [v.reshape(-1, 128) for v in (gate_scale, up_scale, query_scale, key_scale, value_scale, head_gain)]
        + [row(decay_rate)],
    )
    ffn_arrays = gather_ffn(ffn_mine)
    every = lax.all_to_all(copies, ("x", "core"), split_axis=0, concat_axis=0, tiled=True)
    mix_arrays = gather_mix(mix_mine)

    arrived = feed_forward(small, [every], ffn_arrays)
    stream, copies = join(0.5, 1, arrived, stream, gains, rows_as=FFN_TO_MIX)
    own, other = gather_rows(copies)
    arrived = mix(small, own, other, mix_arrays)
    stream, copies = join(1.0, 2, arrived, stream, gains, arrived_as=MIX_TO_FFN)
    rows = gather_rows(copies)
    arrived = feed_forward(small, rows, ffn_arrays)
    return join(0.5, None, arrived, stream, gains)[0]


def solution(mesh):
    devices = mesh.devices
    fine = Mesh(devices.reshape(2, NZ, NY, NX, 2), ("rep", "z", "y", "x", "core"))
    F, T = ("z", "y"), ("x", "core")
    rows = P(("rep", "z", "y", "x", "core"), None)
    wide, tall, cols, depth = P(F, T), P(T, F), P(T), P(F)
    placed = (
        rows, P(), wide, cols, wide, cols, tall, depth,
        wide, cols, wide, cols, wide, cols, tall, depth,
        P(), cols,
    )
    return jax.shard_map(on_device, mesh=fine, in_specs=placed, out_specs=rows, check_vma=False)
```

```python
import math

import jax
import jax.numpy as jnp
from jax import lax
from jax.experimental import pallas as pl
from jax.experimental.pallas import tpu as pltpu
from jax.sharding import Mesh, PartitionSpec as P


DK = 256
BLOCK = 64
EPSILON = 1e-05
NZ, NY, NX = 8, 4, 4
ROWS = 32
VMEM = pl.BlockSpec(memory_space=pltpu.VMEM)


def dot(a, b):
    return jnp.dot(a, b, preferred_element_type=jnp.float32)


def dot_t(a, b):
    return lax.dot_general(a, b, (((1,), (1,)), ((), ())), preferred_element_type=jnp.float32)


def low(w):
    return w.astype(jnp.bfloat16)


NEAR = (0, -1, 1, -2, 2)
DISTANT = (-3, 3, -4)
SIDES = (0, -1, 1, 2)
RING = (0, -1, -2, -3, -4, 1, 2, 3)


def plain(dz, dy):
    return dz % NZ * NY + dy % NY


FFN_ORDER = [plain(dz, dy) for dzs in (NEAR, DISTANT) for dy in SIDES for dz in dzs]
MIX_ORDER = [plain(dz, dy) for dz in RING for dy in range(NY)]
PLAIN_TO_FFN = FFN_ORDER
FFN_TO_PLAIN = [FFN_ORDER.index(b) for b in range(NZ * NY)]
FFN_TO_MIX = [FFN_ORDER.index(b) for b in MIX_ORDER]
MIX_TO_FFN = [MIX_ORDER.index(b) for b in FFN_ORDER]


def joined(tiles):
    (a, turn_a), (b, turn_b) = tiles
    lane = lax.broadcasted_iota(jnp.int32, a.shape, 1)
    a, b = (
        jnp.where(t, pltpu.roll(v, 64, 1), v) if not isinstance(t, bool) else (pltpu.roll(v, 64, 1) if t else v)
        for v, t in ((a, turn_a), (b, turn_b))
    )
    return jnp.where(lane < 64, a, b)


def shuffled(value, order):
    tiles = []
    for p, q in zip(order[::2], order[1::2]):
        a, b = (value[:, i // 2 * 128 : i // 2 * 128 + 128] for i in (p, q))
        tiles.append(joined(((a, p % 2 == 1), (b, q % 2 == 0))))
    return jnp.concatenate(tiles, axis=1)


def turned_in_place(value, y):
    wide = 64 * NY
    shift = lax.rem(wide - 64 * y, wide)
    groups = [value[:, g : g + wide] for g in range(0, value.shape[1], wide)]
    return jnp.concatenate([pltpu.roll(g, shift, 1) for g in groups], axis=1)


def turned(ref, z, y):
    tiles = []
    for t in range(NZ * NY // 2):
        pair = []
        for half in range(2):
            b = 2 * t + half
            side = lax.rem(b % NY + y, NY)
            at = pl.multiple_of((lax.rem(b // NY + z, NZ) * (NY // 2) + side // 2) * 128, 128)
            pair.append((ref[:, pl.ds(at, 128)].astype(jnp.float32), side % 2 != half))
        tiles.append(joined(pair))
    return jnp.concatenate(tiles, axis=1)


def normed(stream, gain):
    scale = lax.rsqrt(jnp.mean(stream * stream, axis=-1, keepdims=True) + EPSILON)
    return low(stream * scale * gain)


def pack_kernel(gate, up, down, ds, query, key, value, out, os, tokens, gains, *rest):
    small, (ffn_ref, mix_ref, rows_ref, small_ref, stream_ref, gains_ref) = rest[:-6], rest[-6:]

    def column(row):
        n = row.shape[1]
        i = lax.broadcasted_iota(jnp.int32, (n, n), 0)
        j = lax.broadcasted_iota(jnp.int32, (n, n), 1)
        return jnp.sum(jnp.where(i == j, row, 0.0), axis=1, keepdims=True)

    def scaled(w, s):
        return low(low(w[...]).astype(jnp.float32) * column(s[...]))

    n = gate.shape[1]
    ffn_ref[:, :n] = low(gate[...])
    ffn_ref[:, n : 2 * n] = low(up[...])
    ffn_ref[:, 2 * n :] = scaled(down, ds)
    mix = (low(query[...]), low(key[...]), low(value[...]), scaled(out, os))
    for k in range(NY):
        for i, w in enumerate(mix):
            mix_ref[k, :, i * DK : (i + 1) * DK] = w
    z, y = lax.axis_index("z"), lax.axis_index("y")
    stream = shuffled(turned(tokens, z, y), PLAIN_TO_FFN)
    ordered = shuffled(turned(gains, z, y), PLAIN_TO_FFN)
    stream_ref[...] = low(stream)
    gains_ref[...] = ordered
    first = normed(stream, ordered[:1, :])
    for k in range(rows_ref.shape[0]):
        rows_ref[k] = first
    for i, v in enumerate(small):
        for k in range(v.shape[0]):
            row = jnp.broadcast_to(v[k : k + 1, :], (1, 128))
            small_ref[i : i + 1, k * 128 : k * 128 + 128] = row


def pack(gate, up, down, ds, query, key, value, out, os, tokens, gains, small):
    rows, n = gate.shape
    return pl.pallas_call(
        pack_kernel,
        out_shape=(
            jax.ShapeDtypeStruct((rows, 3 * n), jnp.bfloat16),
            jax.ShapeDtypeStruct((NY, rows, 4 * DK), jnp.bfloat16),
            jax.ShapeDtypeStruct((NX, *tokens.shape), jnp.bfloat16),
            jax.ShapeDtypeStruct((8, n), jnp.float32),
            jax.ShapeDtypeStruct(tokens.shape, jnp.bfloat16),
            jax.ShapeDtypeStruct(gains.shape, jnp.float32),
        ),
        in_specs=[VMEM] * (11 + len(small)),
        out_specs=(VMEM,) * 6,
        name="pack",
    )(gate, up, down, ds, query, key, value, out, os, tokens, gains, *small)


def join_kernel(weight, which, arrived_as, rows_as, arrived, stream, gains, next_ref, last_ref):
    total = arrived[0].astype(jnp.float32)
    for k in range(1, NX):
        total = total + arrived[k].astype(jnp.float32)
    if arrived_as is not None:
        total = shuffled(turned_in_place(total, lax.axis_index("y")), arrived_as)
    total = stream[...].astype(jnp.float32) + weight * total
    if which is None:
        z, y = lax.axis_index("z"), lax.axis_index("y")
        last_ref[...] = shuffled(total, FFN_TO_PLAIN)
        next_ref[...] = low(turned(last_ref, NZ - z, NY - y))
        return
    next_ref[...] = total
    rows = total * lax.rsqrt(jnp.mean(total * total, axis=-1, keepdims=True) + EPSILON)
    rows = rows * gains[which : which + 1, :]
    if rows_as is not None:
        rows = turned_in_place(shuffled(rows, rows_as), NY - lax.axis_index("y"))
    rows = low(rows)
    for k in range(NX):
        last_ref[k] = rows


def join(weight, which, arrived, stream, gains, arrived_as=None, rows_as=None):
    shape = stream.shape
    last = which is None
    outs = [jax.ShapeDtypeStruct(shape, jnp.bfloat16 if last else jnp.float32)]
    if not last:
        outs.append(jax.ShapeDtypeStruct((NX, *shape), jnp.bfloat16))
    return pl.pallas_call(
        lambda *refs: join_kernel(weight, which, arrived_as, rows_as, *refs),
        out_shape=outs,
        in_specs=[VMEM] * 3,
        out_specs=[VMEM] * len(outs),
        scratch_shapes=[pltpu.VMEM(shape, jnp.float32)] if last else [],
        compiler_params=pltpu.CompilerParams(vmem_limit_bytes=8 * 1024 * 1024),
        name="join",
    )(arrived, stream, gains)


def along_z(array, step):
    return lax.ppermute(array, ("rep", "z"), [(g, (g + step) % (2 * NZ)) for g in range(2 * NZ)])


def along_y(array, step):
    return lax.ppermute(array, "y", [(g, (g + step) % NY) for g in range(NY)])


def gather_ffn(mine):
    u1, d1 = along_z(mine, 1), along_z(mine, -1)
    u2, d2 = along_z(u1, 1), along_z(d1, -1)
    u3, d3 = along_z(u1, 2), along_z(d1, -2)
    u4 = along_z(u2, 2)
    arrays = []

    def spread(blocks, far_up):
        own = jnp.stack(blocks)
        below = along_y(own, 1)
        above = along_y(own, -1)
        far = along_y(below, 1) if far_up else along_y(above, -1)
        arrays.extend((own, below, above, far))

    spread([mine, u1, d1, u2, d2], True)
    spread([u3, d3, u4], False)
    return arrays


def pick_kernel(first, second, out):
    @pl.when(lax.axis_index("core") == 0)
    def _():
        out[...] = first[...]

    @pl.when(lax.axis_index("core") != 0)
    def _():
        out[...] = second[...]


def gather_mix(copies):
    mine = lax.all_to_all(copies, "y", split_axis=0, concat_axis=0, tiled=True)
    mine = mine.reshape(-1, copies.shape[2])

    u1, d1 = along_z(mine, 1), along_z(mine, -1)
    u2, d2 = along_z(u1, 1), along_z(d1, -1)
    d3, u3 = along_z(d1, -2), along_z(u2, 1)
    last = pl.pallas_call(
        pick_kernel,
        out_shape=jax.ShapeDtypeStruct(mine.shape, mine.dtype),
        in_specs=[VMEM, VMEM],
        out_specs=VMEM,
        compiler_params=pltpu.CompilerParams(vmem_limit_bytes=4 * 1024 * 1024),
        name="pick",
    )(u3, d3)
    ring = 2 * NZ
    pairs = [(2 * g + c, 2 * ((g + 1 - 2 * c) % ring) + c) for g in range(ring) for c in (0, 1)]
    last = lax.ppermute(last, ("rep", "z", "core"), pairs)
    return [mine, u1, u2, u3, last, d1, d2, d3]


def swap_cores(array):
    return lax.ppermute(array, "core", [(0, 1), (1, 0)])


def gather_rows(copies):
    own = lax.all_to_all(copies, "x", split_axis=0, concat_axis=0, tiled=True)
    own = own.reshape(-1, copies.shape[2])
    return own, swap_cores(own)


def return_rows(own, other):
    swapped = swap_cores(other)
    both = low(own + swapped.astype(jnp.float32))
    blocks = both.reshape(NX, -1, both.shape[1])
    return lax.all_to_all(blocks, "x", split_axis=0, concat_axis=0, tiled=True)


def stacked(arrays, first, last):
    return jnp.concatenate([a[..., first:last].reshape(-1, last - first) for a in arrays], axis=0)


def ffn_kernel(spans, small, *rest):
    row_refs, arrays, (own_ref, other_ref) = rest[:spans], rest[spans:-2], rest[-2:]
    units = arrays[0].shape[-1] // 3
    rows = jnp.concatenate([r[...] for r in row_refs], axis=0)
    gate = dot(rows, stacked(arrays, 0, units)) * small[0:1, :]
    up = dot(rows, stacked(arrays, units, 2 * units)) * small[1:2, :]
    hidden = low(gate / (1.0 + jnp.exp(-gate)) * up)
    part = dot_t(hidden, stacked(arrays, 2 * units, 3 * units))
    half = own_ref.shape[0]
    own_ref[...] = part[:half]
    other_ref[...] = low(part[half:])


def feed_forward(small, row_arrays, arrays):
    wide = row_arrays[0].shape[-1]
    rows = NX * ROWS
    own_part, other_part = pl.pallas_call(
        lambda *refs: ffn_kernel(len(row_arrays), *refs),
        out_shape=(
            jax.ShapeDtypeStruct((rows, wide), jnp.float32),
            jax.ShapeDtypeStruct((rows, wide), jnp.bfloat16),
        ),
        in_specs=[VMEM] + [VMEM] * len(row_arrays) + [VMEM] * len(arrays),
        out_specs=(VMEM, VMEM),
        compiler_params=pltpu.CompilerParams(vmem_limit_bytes=24 * 1024 * 1024),
        name="ffn",
    )(small, *row_arrays, *arrays)
    return return_rows(own_part, other_part)


def mix_kernel(small, own_rows, other_rows, *rest):
    arrays, (own_ref, other_ref) = rest[:-2], rest[-2:]
    core = lax.axis_index("core")
    rows = jnp.concatenate([own_rows[...], other_rows[...]], axis=0)
    query = low(dot(rows, stacked(arrays, 0, DK)) * small[2:3, :DK])
    key_rows = low(dot(rows, stacked(arrays, DK, 2 * DK)) * small[3:4, :DK] / math.sqrt(DK))
    value = low(dot(rows, stacked(arrays, 2 * DK, 3 * DK)) * small[4:5, :DK])

    total = rows.shape[0]

    def position(axis):
        r = lax.broadcasted_iota(jnp.int32, (total, total), axis)
        half = r // (total // 2)
        side = jnp.where(half == 0, core, 1 - core)
        return (r % (total // 2)) // ROWS * (2 * ROWS) + side * ROWS + r % ROWS

    pi, pj = position(0), position(1)
    apart = jnp.abs(pi - pj).astype(jnp.float32)
    decay = jnp.where(pj // BLOCK <= pi // BLOCK, jnp.exp(-small[6:7, :1] * apart), 0.0)
    scores = low(dot_t(query, key_rows) * decay)
    retained = dot(scores, value)
    centred = retained - jnp.mean(retained, axis=-1, keepdims=True)
    scale = lax.rsqrt(jnp.mean(centred * centred, axis=-1, keepdims=True) + EPSILON)
    mixed = low(centred * scale * small[5:6, :DK])
    part = dot_t(mixed, stacked(arrays, 3 * DK, 4 * DK))
    half = own_ref.shape[0]
    own_ref[...] = part[:half]
    other_ref[...] = low(part[half:])


def mix(small, own, other, arrays):
    rows, wide = own.shape
    own_part, other_part = pl.pallas_call(
        mix_kernel,
        out_shape=(
            jax.ShapeDtypeStruct((rows, wide), jnp.float32),
            jax.ShapeDtypeStruct((rows, wide), jnp.bfloat16),
        ),
        in_specs=[VMEM] * (3 + len(arrays)),
        out_specs=(VMEM, VMEM),
        compiler_params=pltpu.CompilerParams(vmem_limit_bytes=24 * 1024 * 1024),
        name="mix",
    )(small, own, other, *arrays)
    return return_rows(own_part, other_part)


def on_device(
    tokens_in, norm_gains, gate_w, gate_scale, up_w, up_scale, down_w, down_scale,
    query_w, query_scale, key_w, key_scale, value_w, value_scale, out_w, out_scale,
    head_gain, decay_rate,
):
    def row(v):
        return v.reshape(1, -1)

    ffn_mine, mix_mine, copies, small, stream, gains = pack(
        gate_w, up_w, down_w.T, row(down_scale), query_w, key_w, value_w, out_w.T,
        row(out_scale), tokens_in, norm_gains,
        [v.reshape(-1, 128) for v in (gate_scale, up_scale, query_scale, key_scale, value_scale, head_gain)]
        + [row(decay_rate)],
    )
    ffn_arrays = gather_ffn(ffn_mine)
    rows = gather_rows(copies)
    mix_arrays = gather_mix(mix_mine)

    arrived = feed_forward(small, rows, ffn_arrays)
    stream, copies = join(0.5, 1, arrived, stream, gains, rows_as=FFN_TO_MIX)
    own, other = gather_rows(copies)
    arrived = mix(small, own, other, mix_arrays)
    stream, copies = join(1.0, 2, arrived, stream, gains, arrived_as=MIX_TO_FFN)
    rows = gather_rows(copies)
    arrived = feed_forward(small, rows, ffn_arrays)
    return join(0.5, None, arrived, stream, gains)[0]


def solution(mesh):
    devices = mesh.devices
    fine = Mesh(devices.reshape(2, NZ, NY, NX, 2), ("rep", "z", "y", "x", "core"))
    F, T = ("z", "y"), ("x", "core")
    rows = P(("rep", "z", "y", "x", "core"), None)
    wide, tall, cols, depth = P(F, T), P(T, F), P(T), P(F)
    placed = (
        rows, P(), wide, cols, wide, cols, tall, depth,
        wide, cols, wide, cols, wide, cols, tall, depth,
        P(), cols,
    )
    return jax.shard_map(on_device, mesh=fine, in_specs=placed, out_specs=rows, check_vma=False)
```
